32 devices in a mesh: ep: 8 (over z, y), tp: 4 (over x, core).
Axes of the slice: x: 2, y: 2, z: 4, core: 2. Of those that a mesh axis runs over, the one named last changes fastest.
Arguments:
- hidden: bfloat16 [256, 2048], P('ep')
- norm_gains: float32 [4, 2048], replicated, may hold values from 0.1 to 1.9
- w_query: bfloat16 [2048, 1024], P(None, 'tp'), may hold values from -0.125 to 0.125
- w_key: bfloat16 [2048, 1024], P(None, 'tp'), may hold values from -0.125 to 0.125
- w_value: bfloat16 [2048, 1024], P(None, 'tp'), may hold values from -0.125 to 0.125
- w_outgate: bfloat16 [2048, 1024], P(None, 'tp'), may hold values from -0.125 to 0.125
- w_input_gate: bfloat16 [2048, 8], replicated, may hold values from -0.125 to 0.125
- w_forget_gate: bfloat16 [2048, 8], replicated, may hold values from -0.125 to 0.125
- forget_bias: float32 [8], replicated, may hold values from -1 to 4
- w_mix_out: bfloat16 [1024, 2048], P('tp')
- state_matrix: float32 [256, 8, 128, 128], P('ep', 'tp'), may hold values from -0.6 to 0.6
- state_norm: float32 [256, 8, 128], P('ep', 'tp'), may hold values from -0.6 to 0.6
- state_max: float32 [256, 8], P('ep', 'tp'), may hold values from -4 to 4
- routes: int32 [256, 2], P('ep'), may hold values from 0 to 7, all different within a row; in each aligned block of 32 rows (0 to 31, 32 to 63, ...) at most 16 rows name the same one
- route_scores: float32 [256, 2], P('ep'), may hold values from 0.1 to 1
- expert_gate: bfloat16 [8, 2048, 3584], P('ep', None, 'tp'), may hold values from -0.125 to 0.125
- expert_up: bfloat16 [8, 2048, 3584], P('ep', None, 'tp'), may hold values from -0.125 to 0.125
- expert_down: bfloat16 [8, 3584, 2048], P('ep', 'tp')
- dense_gate: bfloat16 [2048, 5632], P('tp', 'ep'), may hold values from -0.125 to 0.125
- dense_up: bfloat16 [2048, 5632], P('tp', 'ep'), may hold values from -0.125 to 0.125
- dense_down: bfloat16 [5632, 2048], P('ep', 'tp')
- dense_mix: float32 [2048], replicated, may hold values from -0.25 to 0.25
Outputs:
- new_hidden: bfloat16 [256, 2048], P('ep', 'tp')
- new_matrix: float32 [256, 8, 128, 128], P('ep', 'tp')
- new_norm: float32 [256, 8, 128], P('ep', 'tp')
- new_max: float32 [256, 8], P('ep', 'tp')
The draws below stay inside these ranges and needn't reach their ends.
Inputs may be any that keep to these rules, and one draw needn't show every extreme that they name: `routes`: each row names 2 different experts. Among the rows of one index of ep (an aligned block of 32 rows) no expert is named by more than 16 rows, and in every draw some expert is named by exactly 16 rows of some block.
All inputs are finite; a program needn't handle non-finite values.
Results may differ from the reference program's by a relative error of at most 0.02.
Values may be sent and summed in bfloat16 or wider, within the bound.
No kernel may reach another device: no remote copies, remote signals or barrier semaphores. Data moves between devices by JAX's collectives and lax.ppermute only.
A program may use at most 128 MiB of HBM per device.

```python
import math
import jax
import jax.numpy as jnp
import numpy as np
from jax import lax

D = 2048
HEADS = 8
HEAD = 128
FF_E = 3584
FF = 5632
TOP = 2
SEQ_DEV = 32
EXPERTS = 8
CAP = 16
SEQS = 256
N_EP = 8
N_TP = 4


def column_scaled(key, array_shape, fan_in, marker):
    noise_key, level_key = jax.random.split(jax.random.fold_in(key, marker))
    columns = array_shape[-1]
    position = jnp.arange(columns, dtype=jnp.float32) / columns
    levels = 0.5 * position + 0.5 * jax.random.uniform(level_key, (columns,), jnp.float32)
    noise = jax.random.normal(noise_key, array_shape, jnp.float32)
    scales = 10.0 ** levels
    scales = scales / jnp.sqrt(jnp.mean(scales * scales))
    return (noise * scales * (1.0 / fan_in) ** 0.5).astype(jnp.bfloat16)


def draw_hidden(key, part):
    return column_scaled(key, (SEQS, D), 1, 101)


def draw_w_mix_out(key, part):
    return column_scaled(key, (HEADS * HEAD, D), HEADS * HEAD, 102)


def draw_expert_down(key, part):
    return column_scaled(key, (EXPERTS, FF_E, D), FF_E, 103)


def draw_dense_down(key, part):
    return column_scaled(key, (FF, D), FF, 104)


def block_levels(rng, shape, cuts, low, top_value):
    gain = 1.0
    for axis_at, parts in cuts:
        heights = jax.random.uniform(jax.random.fold_in(jax.random.fold_in(rng, 6), axis_at), (parts,), jnp.float32, low / len(cuts), top_value / len(cuts))
        gain = gain * jnp.repeat(jnp.exp(heights), shape[axis_at] // parts).reshape((-1,) + (1,) * (len(shape) - 1 - axis_at))
    return gain


def deal_out(own_key, own, number, rows, amount, top, limit, lean):
    order = jax.random.permutation(own_key, amount)
    heavy_load, ordinary = load_shares(amount, rows * top, limit, lean, True), load_shares(amount, rows * top, limit, lean, False)
    places = jnp.arange(amount)

    def named(tallies, rotation):
        used = int((tallies > 0).sum())
        fixed = max(1, used // 4)
        passed = fixed + (places - fixed + rotation * (used - fixed)) % max(1, amount - fixed)
        return jnp.zeros((amount,), jnp.int32).at[order[jnp.where(places < fixed, places, passed)]].set(jnp.asarray(tallies, jnp.int32))

    tallies = jnp.where(number % 4 == 0, named(heavy_load, number // 4), named(ordinary, number - number // 4 - 1))
    mixed = jax.random.permutation(jax.random.fold_in(own, 3), amount)
    giver, sink = mixed[0:amount // 2 * 2:2], mixed[1:amount // 2 * 2:2]
    slack = jnp.minimum(tallies[giver] - 1, limit - tallies[sink]) // 2
    slack = jnp.where((giver == order[0]) | (sink == order[0]) | (tallies[sink] == 0), 0, jnp.maximum(slack, 0))
    passed = jax.random.randint(jax.random.fold_in(own, 4), (amount // 2,), 0, 1 << 20) % (slack + 1)
    tallies = tallies.at[giver].add(-passed).at[sink].add(passed)
    members = jnp.searchsorted(jnp.cumsum(tallies), jnp.arange(rows * top), side="right").astype(jnp.int32)
    table = members.reshape(top, rows).T
    table = table[jax.random.permutation(jax.random.fold_in(own, 1), rows)]
    rotation = jax.random.randint(jax.random.fold_in(own, 2), (rows, 1), 0, top)
    return jnp.take_along_axis(table, (jnp.arange(top)[None, :] + rotation) % top, axis=1)


def load_shares(number_of, total, most, lean, full):
    portions = [(1 << 20) // math.isqrt(standing ** lean) + 1 for standing in range(1, number_of + 1)]
    largest = most if full else min(most, max(-(-total // number_of), total * portions[0] // sum(portions)))
    least = 1 if total - largest >= number_of - 1 else 0
    counts, surplus = [largest] + [least] * (number_of - 1), total - largest - least * (number_of - 1)
    while surplus > 0:
        candidates = [i for i in range(1, number_of) if counts[i] < largest] or [i for i in range(1, number_of) if counts[i] < most]
        pool, left = sum([portions[i] for i in candidates]), surplus
        for i in candidates:
            extra = min(most - counts[i], max(1, left * portions[i] // pool), surplus)
            counts[i] = counts[i] + extra
            surplus = surplus - extra
    return np.array(counts)


def normal_values(rng, dims, deviation, reach, shards=(), held_as=jnp.bfloat16):
    values = jax.random.normal(rng, dims, jnp.float32) * deviation
    if len(shards) > 0:
        values = block_levels(rng, dims, shards, -0.22, 0.18) * values
    return jnp.clip(values, min=-reach, max=reach).astype(held_as)


def setup_inputs(seed: int = 0) -> dict:
    arg_keys = jax.random.split(jax.random.key(seed), 23)
    hidden = draw_hidden(jax.random.fold_in(arg_keys[22], 71), 0)
    norm_gains = jnp.clip(1.0 + 0.18 * jax.random.normal(arg_keys[1], (4, D), jnp.float32), 0.1, 1.9)
    w_query = normal_values(arg_keys[2], (D, HEADS * HEAD), D ** -0.5, 0.125, ((1, 4),))
    w_key = normal_values(arg_keys[3], (D, HEADS * HEAD), D ** -0.5, 0.125, ((1, 4),))
    w_value = normal_values(arg_keys[4], (D, HEADS * HEAD), D ** -0.5, 0.125, ((1, 4),))
    w_outgate = normal_values(arg_keys[5], (D, HEADS * HEAD), D ** -0.5, 0.125, ((1, 4),))
    w_input_gate = normal_values(arg_keys[6], (D, HEADS), D ** -0.5, 0.125)
    w_forget_gate = normal_values(arg_keys[7], (D, HEADS), D ** -0.5, 0.125)
    forget_bias = jnp.clip(jax.random.uniform(arg_keys[8], (HEADS,), jnp.float32, -1.0, 4.0), -1.0, 4.0)
    w_mix_out = draw_w_mix_out(jax.random.fold_in(arg_keys[22], 71), 0)
    state_matrix = normal_values(arg_keys[10], (SEQS, HEADS, HEAD, HEAD), 0.1, 0.6, ((0, 8), (1, 4)), jnp.float32)
    state_norm = normal_values(arg_keys[11], (SEQS, HEADS, HEAD), 0.1, 0.6, ((0, 8), (1, 4)), jnp.float32)
    state_max = normal_values(arg_keys[12], (SEQS, HEADS), 1.0, 4.0, ((0, 8), (1, 4)), jnp.float32)
    routes_keys = jax.random.split(jax.random.fold_in(arg_keys[13], 1), SEQS // SEQ_DEV)
    routes_turns = jax.random.permutation(jax.random.fold_in(arg_keys[13], 3), SEQS // SEQ_DEV)
    routes = jax.vmap(lambda own, number: deal_out(jax.random.fold_in(arg_keys[13], 2), own, number, SEQ_DEV, EXPERTS, TOP, CAP, 2))(routes_keys, routes_turns).reshape((SEQS, TOP))
    route_scores = jnp.clip(jnp.exp(math.log(1.0) - 2.3025851 * jax.random.uniform(arg_keys[14], (SEQS, TOP), jnp.float32) ** block_levels(arg_keys[14], (SEQS, TOP), ((0, 8),), -0.2, 0.2)), 0.1, 1.0)
    expert_gate = normal_values(arg_keys[15], (EXPERTS, D, FF_E), D ** -0.5, 0.125, ((0, 8), (2, 4)))
    expert_up = normal_values(arg_keys[16], (EXPERTS, D, FF_E), D ** -0.5, 0.125, ((0, 8), (2, 4)))
    expert_down = draw_expert_down(jax.random.fold_in(arg_keys[22], 71), 0)
    dense_gate = normal_values(arg_keys[18], (D, FF), D ** -0.5, 0.125, ((0, 4), (1, 8)))
    dense_up = normal_values(arg_keys[19], (D, FF), D ** -0.5, 0.125, ((0, 4), (1, 8)))
    dense_down = draw_dense_down(jax.random.fold_in(arg_keys[22], 71), 0)
    dense_mix = normal_values(arg_keys[21], (D,), (D // 4) ** -0.5, 0.25, (), jnp.float32)
    return dict(hidden=hidden, norm_gains=norm_gains, w_query=w_query, w_key=w_key, w_value=w_value, w_outgate=w_outgate, w_input_gate=w_input_gate, w_forget_gate=w_forget_gate, forget_bias=forget_bias, w_mix_out=w_mix_out, state_matrix=state_matrix, state_norm=state_norm, state_max=state_max, routes=routes, route_scores=route_scores, expert_gate=expert_gate, expert_up=expert_up, expert_down=expert_down, dense_gate=dense_gate, dense_up=dense_up, dense_down=dense_down, dense_mix=dense_mix)


EPS = 1e-06

def inverse_rms(values):
    return lax.rsqrt(lax.optimization_barrier(jnp.mean(values * values, axis=-1, keepdims=True)) + EPS)

def settle(values):
    return lax.optimization_barrier(values.astype(jnp.bfloat16)).astype(jnp.float32)

def grouped_product(activations, weights_in):
    row_count, inner_width = activations.shape
    group_width = inner_width // N_TP
    left_side = activations.astype(jnp.float32).reshape(row_count, N_TP, group_width)
    right_side = weights_in.astype(jnp.float32).reshape(N_TP, group_width, weights_in.shape[1])
    pieces = settle(jnp.einsum('rbf,bfd->brd', left_side, right_side))
    return lax.optimization_barrier(jnp.sum(pieces, axis=0)).astype(jnp.bfloat16)

def reference(hidden, norm_gains, w_query, w_key, w_value, w_outgate, w_input_gate, w_forget_gate, forget_bias, w_mix_out, state_matrix, state_norm, state_max, routes, route_scores, expert_gate, expert_up, expert_down, dense_gate, dense_up, dense_down, dense_mix):
    start_f = hidden.astype(jnp.float32)
    normed_in = (start_f * inverse_rms(start_f) * norm_gains[0]).astype(jnp.bfloat16)

    def project(weight):
        return settle(jnp.dot(normed_in, weight, preferred_element_type=jnp.float32))
    query = project(w_query).reshape(SEQS, HEADS, HEAD)
    keys = project(w_key).reshape(SEQS, HEADS, HEAD) * HEAD ** (-0.5)
    values = project(w_value).reshape(SEQS, HEADS, HEAD)
    out_gate = project(w_outgate)
    in_gate = jnp.dot(normed_in, w_input_gate, preferred_element_type=jnp.float32)
    log_forget = jax.nn.log_sigmoid(jnp.dot(normed_in, w_forget_gate, preferred_element_type=jnp.float32) + forget_bias)
    carried = log_forget + state_max
    new_max = jnp.maximum(carried, in_gate)
    keep = jnp.exp(carried - new_max)
    write = jnp.exp(in_gate - new_max)
    written = write[:, :, None] * keys
    new_matrix = keep[:, :, None, None] * state_matrix + written[:, :, :, None] * values[:, :, None, :]
    new_norm = keep[:, :, None] * state_norm + written
    numer = jnp.einsum('shd,shdv->shv', query, new_matrix)
    denom = jnp.einsum('shd,shd->sh', query, new_norm)
    read = numer / jnp.maximum(jnp.abs(denom), jnp.exp(-new_max))[:, :, None]
    mixed = (jax.nn.sigmoid(out_gate) * read.reshape(SEQS, HEADS * HEAD)).astype(jnp.bfloat16)
    branch = settle(grouped_product(mixed, w_mix_out))
    residual_f = start_f + norm_gains[1] * branch * inverse_rms(branch)
    residual = settle(residual_f)
    scale_two = inverse_rms(residual_f)
    normed = (residual_f * scale_two * norm_gains[2]).astype(jnp.bfloat16)
    mix_gate = jax.nn.sigmoid(scale_two[:, 0] * lax.optimization_barrier(jnp.sum(residual_f * norm_gains[2] * dense_mix, axis=-1)))
    dense_pre_gate = jnp.dot(normed, dense_gate, preferred_element_type=jnp.float32)
    dense_pre_up = jnp.dot(normed, dense_up, preferred_element_type=jnp.float32)
    dense_hidden = (jax.nn.silu(dense_pre_gate) * dense_pre_up).astype(jnp.bfloat16)
    dense_out = jnp.dot(dense_hidden, dense_down, preferred_element_type=jnp.float32)
    pairs = routes.reshape(N_EP, SEQ_DEV * TOP).astype(jnp.int32)
    picks = (pairs[:, :, None] == jnp.arange(EXPERTS, dtype=jnp.int32)[None, None, :]).astype(jnp.int32)
    ranks = (lax.optimization_barrier(jnp.sum(jnp.cumsum(picks, axis=1) * picks, axis=-1)) - 1).astype(jnp.int32)
    buffer_row = (jnp.arange(N_EP, dtype=jnp.int32)[:, None] * CAP + ranks).reshape(-1).astype(jnp.int32)
    flat_expert = pairs.reshape(-1)
    token_index = (jnp.arange(SEQS * TOP, dtype=jnp.int32) // TOP).astype(jnp.int32)
    expert_in = jnp.zeros((EXPERTS, N_EP * CAP, D), jnp.bfloat16).at[flat_expert, buffer_row].set(normed[token_index])

    def run_expert(operands):
        inputs, gate_weight, up_weight, down_weight = operands
        gate_pre = jnp.dot(inputs, gate_weight, preferred_element_type=jnp.float32)
        up_pre = jnp.dot(inputs, up_weight, preferred_element_type=jnp.float32)
        hidden_units = (jax.nn.silu(gate_pre) * up_pre).astype(jnp.bfloat16)
        return grouped_product(hidden_units, down_weight)
    expert_out = lax.map(run_expert, (expert_in, expert_gate, expert_up, expert_down))
    picked = settle(expert_out[flat_expert, buffer_row]).reshape(SEQS, TOP, D)
    share = route_scores / lax.optimization_barrier(jnp.sum(route_scores, axis=-1, keepdims=True))
    ffn = lax.optimization_barrier(jnp.sum(share[:, :, None] * picked, axis=1)) + mix_gate[:, None] * dense_out
    new_hidden = (residual + norm_gains[3] * ffn * inverse_rms(ffn)).astype(jnp.bfloat16)
    return (new_hidden, new_matrix, new_norm, new_max)
```

```python
import jax
import jax.numpy as jnp
from jax import lax
from jax.sharding import PartitionSpec as P

EPS = 1e-06
F32 = jnp.float32
BF16 = jnp.bfloat16


def settle(values):
    return lax.optimization_barrier(values.astype(BF16)).astype(F32)


def dot(left, right):
    return jnp.dot(left, right, preferred_element_type=F32)


def swap(values, axis, step):
    count = lax.axis_size(axis)
    return lax.ppermute(values, axis, [(i, i ^ step) for i in range(count)])


def gather_own_first(values, axis):
    return [values] + [swap(values, axis, j) for j in range(1, lax.axis_size(axis))]


def in_order(pieces, place):
    stacked = jnp.stack(pieces)
    return [
        lax.dynamic_index_in_dim(stacked, place ^ j, 0, keepdims=False) for j in range(len(pieces))
    ]


def add_pieces(pieces):
    total = pieces[0].astype(F32)
    for piece in pieces[1:]:
        total = total + piece.astype(F32)
    return total


def steps_of(count):
    steps, step = [], count // 2
    while step:
        steps.append(step)
        step //= 2
    return steps


def three_parts(values):
    high = lax.reduce_precision(values, 8, 7)
    rest = values - high
    middle = lax.reduce_precision(rest, 8, 7)
    return [high, middle, rest - middle]


def local(
    hidden,
    norm_gains,
    w_query,
    w_key,
    w_value,
    w_outgate,
    w_input_gate,
    w_forget_gate,
    forget_bias,
    w_mix_out,
    state_matrix,
    state_norm,
    state_max,
    routes,
    route_scores,
    expert_gate,
    expert_up,
    expert_down,
    dense_gate,
    dense_up,
    dense_down,
    dense_mix,
):
    tp_count = lax.axis_size("tp")
    ep_count = lax.axis_size("ep")
    tp_place = lax.axis_index("tp")
    ep_place = lax.axis_index("ep")
    seq_local, width = hidden.shape
    heads_local = state_matrix.shape[1]
    head_width = state_matrix.shape[2]
    part_width = width // tp_count
    feature_first = tp_place * part_width
    route_width = routes.shape[1]
    capacity = 2 * seq_local * route_width // ep_count

    flat_expert = routes.reshape(-1)
    pair = jnp.arange(flat_expert.shape[0], dtype=jnp.int32)
    ranks = jnp.sum(
        (
            (flat_expert[:, None] == flat_expert[None, :]) & (pair[None, :] < pair[:, None])
        ).astype(jnp.int32),
        axis=1,
    ).reshape(routes.shape)
    share = route_scores / jnp.sum(route_scores, axis=-1, keepdims=True)

    start_f = hidden.astype(F32)
    normed_in = (
        start_f
        * lax.rsqrt(jnp.mean(start_f * start_f, axis=-1, keepdims=True) + EPS)
        * norm_gains[0]
    ).astype(BF16)
    query_f = dot(normed_in, w_query)
    key_f = dot(normed_in, w_key)
    value_f = dot(normed_in, w_value)
    gate_f = dot(normed_in, w_outgate)
    head_first = tp_place * heads_local
    input_weight = lax.dynamic_slice_in_dim(w_input_gate, head_first, heads_local, 1)
    forget_weight = lax.dynamic_slice_in_dim(w_forget_gate, head_first, heads_local, 1)
    forget_local = lax.dynamic_slice_in_dim(forget_bias, head_first, heads_local, 0)
    in_gate = dot(normed_in, input_weight)
    log_forget = jax.nn.log_sigmoid(dot(normed_in, forget_weight) + forget_local)
    query = settle(query_f).reshape(seq_local, heads_local, head_width)
    keys = settle(key_f).reshape(seq_local, heads_local, head_width) * head_width ** (-0.5)
    values = settle(value_f).reshape(seq_local, heads_local, head_width)
    carried = log_forget + state_max
    new_max = jnp.maximum(carried, in_gate)
    keep = jnp.exp(carried - new_max)
    write = jnp.exp(in_gate - new_max)
    written = write[:, :, None] * keys
    new_matrix = (
        keep[:, :, None, None] * state_matrix + written[:, :, :, None] * values[:, :, None, :]
    )
    new_norm = keep[:, :, None] * state_norm + written
    numer = jnp.einsum("shd,shdv->shv", query, new_matrix)
    denom = jnp.einsum("shd,shd->sh", query, new_norm)
    read = numer / jnp.maximum(jnp.abs(denom), jnp.exp(-new_max))[:, :, None]
    mixed = (
        jax.nn.sigmoid(settle(gate_f)) * read.reshape(seq_local, heads_local * head_width)
    ).astype(BF16)
    branch_terms = lax.optimization_barrier(dot(mixed, w_mix_out).astype(BF16))

    branch = settle(add_pieces(gather_own_first(branch_terms, "tp")))
    branch_scale = lax.rsqrt(jnp.mean(branch * branch, axis=-1, keepdims=True) + EPS)
    residual_f = start_f + norm_gains[1] * branch * branch_scale
    scale_two = lax.rsqrt(jnp.mean(residual_f * residual_f, axis=-1, keepdims=True) + EPS)
    gained = residual_f * norm_gains[2]
    mix_gate = jax.nn.sigmoid(
        scale_two * jnp.sum(gained * dense_mix, axis=-1, keepdims=True)
    )
    residual_part = settle(lax.dynamic_slice_in_dim(residual_f, feature_first, part_width, 1))
    normed = (
        lax.dynamic_slice_in_dim(gained, feature_first, part_width, 1) * scale_two
    ).astype(BF16)

    numbers = [routes.astype(F32), ranks.astype(F32)] + three_parts(share) + three_parts(mix_gate)
    notes = jnp.concatenate(numbers, axis=1).astype(BF16)
    notes = jnp.pad(notes, ((0, 0), (0, 128 - notes.shape[1])))
    blocks = jnp.concatenate([normed, notes], axis=1)[None]
    ep_steps = steps_of(ep_count)
    for step in ep_steps:
        blocks = jnp.concatenate([blocks, swap(blocks, "ep", step)], axis=0)
    rows_all = ep_count * seq_local
    rows_in = blocks[:, :, :part_width].reshape(rows_all, part_width)
    notes_in = blocks[:, :, part_width:].reshape(rows_all, 128).astype(F32)
    route_in = notes_in[:, :route_width]
    rank_in = notes_in[:, route_width : 2 * route_width]
    shares = [
        notes_in[:, route_width * k : route_width * (k + 1)] for k in range(2, 5)
    ]
    share_in = shares[0] + shares[1] + shares[2]
    mix_at = 5 * route_width
    mix_in = (
        notes_in[:, mix_at : mix_at + 1]
        + notes_in[:, mix_at + 1 : mix_at + 2]
        + notes_in[:, mix_at + 2 : mix_at + 3]
    )
    here = (route_in == ep_place.astype(F32)).astype(F32)
    block_first = (jnp.arange(rows_all, dtype=jnp.int32) // seq_local * capacity).astype(F32)
    named = jnp.sum(here, axis=1)
    slot_in = jnp.where(
        named > 0, jnp.sum(here * rank_in, axis=1) + block_first, -1.0
    )
    weight_in = jnp.sum(here * share_in, axis=1, keepdims=True)
    slots = ep_count * capacity
    placing = (
        jnp.arange(slots, dtype=jnp.int32).astype(F32)[:, None] == slot_in[None, :]
    ).astype(BF16)

    expert_rows = dot(placing, rows_in).astype(BF16)
    flat_rows = jnp.concatenate(
        in_order(gather_own_first(expert_rows, "tp"), tp_place), axis=1
    )

    dense_rows = rows_all // tp_count
    dense_pre = jnp.concatenate([dot(rows_in, dense_gate), dot(rows_in, dense_up)], axis=1)
    dense_pre = dense_pre.astype(BF16).reshape(tp_count, dense_rows, -1)
    pre_pieces = [
        lax.dynamic_index_in_dim(dense_pre, tp_place ^ j, 0, keepdims=False)
        for j in range(tp_count)
    ]
    pre_sum = add_pieces(
        [pre_pieces[0]] + [swap(pre_pieces[j], "tp", j) for j in range(1, tp_count)]
    )
    pre_gate, pre_up = jnp.split(pre_sum, 2, axis=1)
    dense_own = (jax.nn.silu(pre_gate) * pre_up).astype(BF16)
    dense_hidden = jnp.concatenate(
        in_order(gather_own_first(dense_own, "tp"), tp_place), axis=0
    )

    gate_pre = dot(flat_rows, expert_gate[0])
    up_pre = dot(flat_rows, expert_up[0])
    hidden_units = (jax.nn.silu(gate_pre) * up_pre).astype(BF16)
    partial_out = lax.optimization_barrier(dot(hidden_units, expert_down[0]).astype(BF16))
    out_pieces = [
        lax.dynamic_slice_in_dim(partial_out, (tp_place ^ j) * part_width, part_width, 1)
        for j in range(tp_count)
    ]
    expert_out = add_pieces(
        [out_pieces[0]] + [swap(out_pieces[j], "tp", j) for j in range(1, tp_count)]
    ).astype(BF16)

    picked = lax.dot_general(
        placing, expert_out, (((0,), (0,)), ((), ())), preferred_element_type=F32
    )
    given = weight_in * picked + mix_in * dot(dense_hidden, dense_down)
    given = given.reshape(ep_count, seq_local, part_width)
    for step in reversed(ep_steps):
        half = given.shape[0] // 2
        given = given[:half] + swap(given[half:].astype(BF16), "ep", step).astype(F32)
    ffn = given[0]
    ffn_sq = jnp.broadcast_to(jnp.sum(ffn * ffn, axis=-1, keepdims=True), (seq_local, 128))
    ffn_sq = add_pieces(gather_own_first(ffn_sq, "tp"))[:, :1]
    gain_last = lax.dynamic_slice_in_dim(norm_gains[3], feature_first, part_width, 0)
    new_hidden = (residual_part + gain_last * ffn * lax.rsqrt(ffn_sq / width + EPS)).astype(BF16)
    return (new_hidden, new_matrix, new_norm, new_max)


def solution(mesh):
    placed = (
        P("ep", None),
        P(),
        P(None, "tp"),
        P(None, "tp"),
        P(None, "tp"),
        P(None, "tp"),
        P(),
        P(),
        P(),
        P("tp", None),
        P("ep", "tp", None, None),
        P("ep", "tp", None),
        P("ep", "tp"),
        P("ep", None),
        P("ep", None),
        P("ep", None, "tp"),
        P("ep", None, "tp"),
        P("ep", "tp", None),
        P("tp", "ep"),
        P("tp", "ep"),
        P("ep", "tp"),
        P(),
    )
    return jax.shard_map(
        local,
        mesh=mesh,
        in_specs=placed,
        out_specs=(P("ep", "tp"), P("ep", "tp", None, None), P("ep", "tp", None), P("ep", "tp")),
        check_vma=False,
    )
```
